32 devices in a mesh: sp: 8 (over z, x), dp: 4 (over y, core).
Axes of the slice: x: 2, y: 2, z: 4, core: 2. Of those that a mesh axis runs over, the one named last changes fastest.
Arguments:
- tokens: bfloat16 [4, 4096, 2048], P('dp', 'sp'), may hold values from -6 to 6
- segments: int32 [4, 4096], P('dp', 'sp'), may hold values from 0 to 3, never falling along the last dimension, each value on 1 to 2048 neighbouring positions
- w_lin: bfloat16 [2048, 1024], P('dp'), may hold values from -0.125 to 0.125
- w_gate: bfloat16 [2048, 1024], P('dp'), may hold values from -0.125 to 0.125
- w_out: bfloat16 [1024, 2048], P(None, 'dp'), may hold values from -0.1875 to 0.1875
- conv_kernel: float32 [31, 1024], replicated, may hold values from -1 to 1
- conv_bias: float32 [1024], replicated, may hold values from -3 to 3
- norm_gain: float32 [1024], replicated, may hold values from 0.1 to 1.9
- norm_bias: float32 [1024], replicated, may hold values from -3 to 3
Outputs:
- mixed_out: bfloat16 [4, 4096, 2048], P('dp', 'sp')
The draws below stay inside these ranges and needn't reach their ends.
Inputs may be any that keep to these rules, and one draw needn't show every extreme that they name: `segments`: within each sequence document numbers never fall; a document is a run of equal numbers of at most four times 512 positions.
All inputs are finite; a program needn't handle non-finite values.
Results may differ from the reference program's by a relative error of at most 0.0062.
Values may be sent and summed in bfloat16 or wider, within the bound.
No kernel may reach another device: no remote copies, remote signals or barrier semaphores. Data moves between devices by JAX's collectives and lax.ppermute only.
A program may use at most 64 MiB of HBM per device.

```python
import math
import jax
import jax.numpy as jnp
import numpy as np
from jax import lax

D = 2048
CW = 1024
K = 31
TOK_DEV = 512
SEQ = 4096
SEQS = 4
N_SP = 8


def steps_of(stream_key, shape, cuts, least, high):
    factor_of, own = 1.0, jax.random.fold_in(stream_key, 6)
    for axis_at, parts in cuts:
        heights = jnp.exp(jax.random.uniform(jax.random.fold_in(own, axis_at), (parts,), jnp.float32, least / len(cuts), high / len(cuts)))
        factor_of = factor_of * jnp.repeat(heights, shape[axis_at] // parts).reshape([-1 if axis == axis_at else 1 for axis in range(len(shape))])
    return factor_of


def length_profile(number_of, total, reach, slope):
    weights = [(1 << 20) // math.isqrt(grade ** slope) + 1 for grade in range(2, number_of + 1)]
    spare, holding = total - reach - (number_of - 1), [1] * (number_of - 1)
    while spare > 0:
        candidates = [i for i in range(number_of - 1) if holding[i] < reach]
        whole, remaining = sum([weights[i] for i in candidates]), spare
        for i in candidates:
            extra = min(reach - holding[i], max(1, remaining * weights[i] // whole), spare)
            holding[i] = holding[i] + extra
            spare = spare - extra
    return np.array([reach] + holding)


def uneven_parts(own_key, count, total, bound, lean):
    if count == 2:
        one = jax.random.randint(own_key, (), max(1, total - bound), min(bound, total - 1) + 1)
        return jnp.stack([one, total - one])
    sizes = jnp.asarray(length_profile(count, total, bound, lean), jnp.int32)
    couples = (count - 1) // 2
    source_of, receiver = sizes[1:1 + 2 * couples:2], sizes[2:2 + 2 * couples:2]
    room = jnp.minimum(source_of - 1, bound - receiver)
    moved = jax.random.randint(jax.random.fold_in(own_key, 1), (couples,), 0, 1 << 20) % (room + 1)
    sizes = sizes.at[1:1 + 2 * couples:2].set(source_of - moved).at[2:2 + 2 * couples:2].set(receiver + moved)
    return sizes[jax.random.permutation(jax.random.fold_in(own_key, 2), count)]


def normal_values(rng, dims, width, limit, cuts=(), held_as=jnp.bfloat16):
    drawn = width * jax.random.normal(rng, dims, jnp.float32)
    if cuts:
        drawn = drawn * steps_of(rng, dims, cuts, -0.22, 0.18)
    return jnp.clip(drawn, -limit, limit).astype(held_as)


def setup_inputs(seed: int = 0) -> dict:
    streams_of = jax.random.split(jax.random.key(seed), 10)
    return {
        "tokens": normal_values(streams_of[0], (SEQS, SEQ, D), 1.0, 6.0, ((0, 4), (1, 8))),
        "segments": jax.vmap(lambda own: jnp.searchsorted(jnp.cumsum(uneven_parts(own, N_SP // 2, SEQ, 4 * TOK_DEV, 2)), jnp.arange(SEQ), side="right"))(jax.random.split(streams_of[1], SEQS)).reshape((SEQS, SEQ)).astype(jnp.int32),
        "w_lin": normal_values(streams_of[2], (D, CW), D ** -0.5, 0.125, ((0, 4),)),
        "w_gate": normal_values(streams_of[3], (D, CW), D ** -0.5, 0.125, ((0, 4),)),
        "w_out": normal_values(streams_of[4], (CW, D), CW ** -0.5, 0.1875, ((1, 4),)),
        "conv_kernel": normal_values(streams_of[5], (K, CW), K ** -0.5, 1.0, (), jnp.float32),
        "conv_bias": normal_values(streams_of[6], (CW,), 0.5, 3.0, (), jnp.float32),
        "norm_gain": jnp.clip(1.0 + 0.18 * jax.random.normal(streams_of[7], (CW,), jnp.float32), 0.1, 1.9),
        "norm_bias": normal_values(streams_of[8], (CW,), 0.5, 3.0, (), jnp.float32),
    }


def conv_doc(values, doc_ids, kernel, bias):
    length = values.shape[1]
    taps = kernel.shape[0]
    total = bias[:, None] + kernel[taps - 1][:, None] * values
    for back in range(1, taps):
        shifted = jnp.pad(values[:, :length - back], ((0, 0), (back, 0)))
        same = jnp.pad(doc_ids[back:] == doc_ids[:length - back], (back, 0))
        total = total + kernel[taps - 1 - back][:, None] * jnp.where(same[None, :], shifted, 0.0)
    return total

def reference(tokens, segments, w_lin, w_gate, w_out, conv_kernel, conv_bias, norm_gain, norm_bias):

    def one_sequence(pair):
        rows, doc_ids = pair
        lin = jnp.dot(rows, w_lin, preferred_element_type=jnp.float32)
        gate = jnp.dot(rows, w_gate, preferred_element_type=jnp.float32)
        glu = (lin * jax.nn.sigmoid(gate)).astype(jnp.bfloat16)
        conv = conv_doc(glu.T.astype(jnp.float32), doc_ids, conv_kernel, conv_bias)
        values = lax.optimization_barrier(conv.astype(jnp.bfloat16)).astype(jnp.float32)
        mean = lax.optimization_barrier(jnp.mean(values, axis=0, keepdims=True))
        var = lax.optimization_barrier(jnp.mean(jnp.square(values - mean), axis=0, keepdims=True))
        normed = (values - mean) * lax.rsqrt(var + 1e-05) * norm_gain[:, None] + norm_bias[:, None]
        act = jax.nn.silu(normed).astype(jnp.bfloat16)
        return jnp.dot(act.T, w_out, preferred_element_type=jnp.float32).astype(jnp.bfloat16)
    return lax.map(one_sequence, (tokens, segments))
```

```python
import functools

import jax
import jax.numpy as jnp
from jax import lax
from jax.experimental import pallas as pl
from jax.experimental.pallas import tpu as pltpu
from jax.sharding import PartitionSpec as P

K = 31
HALO = 32
BLOCK = 8
LANES = 128
AXES = ("sp", "dp")
ANY = pl.BlockSpec(memory_space=pl.ANY)
VMEM = pl.BlockSpec(memory_space=pltpu.VMEM)
SMEM = pl.BlockSpec(memory_space=pltpu.SMEM)


def from_behind(value, axis, by):
    devices = lax.axis_size(axis)
    pairs = [(i, i + by) for i in range(devices) if 0 <= i + by < devices]
    return lax.ppermute(value, axis, pairs)


def conv_doc(values, doc_ids, kernel, bias):
    taps = kernel.shape[0]
    reach = taps - 1
    length = values.shape[1]
    place = lax.iota(jnp.int32, length)
    change = jnp.concatenate([jnp.ones((1,), jnp.bool_), doc_ids[1:] != doc_ids[:-1]])
    begins = lax.cummax(jnp.where(change, place, 0), axis=0)[reach:]
    here = place[reach:]
    total = bias[:, None] + kernel[reach][:, None] * values[:, reach:].astype(jnp.float32)
    for back in range(1, taps):
        piece = values[:, reach - back : length - back].astype(jnp.float32)
        keep = here - back >= begins
        total = total + kernel[reach - back][:, None] * jnp.where(keep[None, :], piece, 0.0)
    return total


def plain_body(tokens, segments, w_lin, w_gate, w_out, conv_kernel, conv_bias, norm_gain, norm_bias):
    rows = tokens[0]
    doc_ids = segments[0]
    count = rows.shape[0]
    reach = K - 1
    first = jnp.einsum(
        "rc,tr->ct",
        lax.all_gather(w_lin, "dp", axis=0, tiled=True),
        rows,
        preferred_element_type=jnp.float32,
    )
    second = jnp.einsum(
        "rc,tr->ct",
        lax.all_gather(w_gate, "dp", axis=0, tiled=True),
        rows,
        preferred_element_type=jnp.float32,
    )
    glu = (first * jax.nn.sigmoid(second)).astype(jnp.bfloat16)
    tail, tail_ids = from_behind((glu[:, count - reach :], doc_ids[count - reach :]), "sp", 1)
    extended = jnp.concatenate([tail, glu], axis=1)
    ext_ids = jnp.concatenate([tail_ids, doc_ids], axis=0)
    conv = conv_doc(extended, ext_ids, conv_kernel, conv_bias)
    conved = lax.optimization_barrier(conv.astype(jnp.bfloat16))
    values = conved.astype(jnp.float32)
    mean = jnp.mean(values, axis=0, keepdims=True)
    var = jnp.mean(jnp.square(values - mean), axis=0, keepdims=True)
    normed = (values - mean) * lax.rsqrt(var + 1e-05) * norm_gain[:, None] + norm_bias[:, None]
    act = jax.nn.silu(normed).astype(jnp.bfloat16)
    mixed_out = jnp.einsum(
        "ct,cr->tr",
        act,
        lax.all_gather(w_out, "dp", axis=1, tiled=True),
        preferred_element_type=jnp.float32,
    ).astype(jnp.bfloat16)
    return mixed_out[None]


def copy_all(copies):
    for c in copies:
        c.start()
    return copies


def wait_all(copies):
    for c in copies:
        c.wait()


def dot(a, b):
    return jnp.dot(a, b, preferred_element_type=jnp.float32)


def near_kernel(place, tokens, halo, l0, g0, l1, g1, acc, x, w, sems):
    shard, width = l0.shape
    count = tokens.shape[0]
    core = place[1]
    half = pl.multiple_of(place[0] * (2 * shard), 2 * shard)
    mine = pl.multiple_of(core * shard, shard)
    other = pl.multiple_of((1 - core) * shard, shard)
    pairs = [
        (tokens.at[:, pl.ds(half, 2 * shard)], x.at[pl.ds(HALO, count)]),
        (halo.at[:, pl.ds(half, 2 * shard)], x.at[pl.ds(0, HALO)]),
        (l0, w.at[pl.ds(mine, shard), pl.ds(0, width)]),
        (g0, w.at[pl.ds(mine, shard), pl.ds(width, width)]),
        (l1, w.at[pl.ds(other, shard), pl.ds(0, width)]),
        (g1, w.at[pl.ds(other, shard), pl.ds(width, width)]),
    ]
    wait_all(copy_all([pltpu.make_async_copy(s, d, sems.at[i]) for i, (s, d) in enumerate(pairs)]))

    def step(n, carry):
        cols = pl.ds(pl.multiple_of(n * 256, 256), 256)
        acc[:, cols] = dot(x[...], w[:, cols])
        return carry

    lax.fori_loop(0, 2 * width // 256, step, 0)


def far_kernel(layout, place, since, least, tokens, halo, acc, taps, bias, gain, nbias, *rest):
    npieces = len(layout)
    pieces = rest[: 2 * npieces]
    act, x, w, glu, conv, sems = rest[2 * npieces :]
    shard = w.shape[0] // 2
    width = act.shape[1]
    count = tokens.shape[0]
    tiles = width // LANES
    half = pl.multiple_of((1 - place[0]) * (2 * shard), 2 * shard)
    pairs = [
        (tokens.at[:, pl.ds(half, 2 * shard)], x.at[pl.ds(HALO, count)]),
        (halo.at[:, pl.ds(half, 2 * shard)], x.at[pl.ds(0, HALO)]),
    ]
    for i, (swap, flip, base, pitch, size) in enumerate(layout):
        core = 1 - place[1] if swap else place[1]
        side = 1 - place[2] if flip else place[2]
        row = pl.multiple_of(core * shard + side * pitch + base, 16)
        for j in range(2):
            pairs.append((pieces[2 * i + j], w.at[pl.ds(row, size), pl.ds(j * width, width)]))
    wait_all(copy_all([pltpu.make_async_copy(s, d, sems.at[i]) for i, (s, d) in enumerate(pairs)]))

    step_cols = 256

    def project(n, carry):
        at = pl.multiple_of(n * step_cols, step_cols)
        cols = pl.ds(at, step_cols)
        gcols = pl.ds(pl.multiple_of(width + at, step_cols), step_cols)
        lin = acc[:, cols] + dot(x[...], w[:, cols])
        gate = acc[:, gcols] + dot(x[...], w[:, gcols])
        value = (lin * jax.nn.sigmoid(gate)).astype(jnp.bfloat16).astype(jnp.float32)
        for j in range(step_cols // LANES):
            glu[pl.ds(n * (step_cols // LANES) + j, count + HALO, stride=tiles), :] = value[
                :, j * LANES : (j + 1) * LANES
            ]
        return carry

    lax.fori_loop(0, width // step_cols, project, 0)

    def row_at(i):
        return glu[pl.ds(pl.multiple_of(i * tiles, tiles), tiles), :]

    def tap(k):
        return taps[pl.ds(k * tiles, tiles), :]

    def convolve(b, carry):
        first = b * BLOCK

        def finish(totals):
            for t in range(BLOCK):
                value = totals[t].astype(jnp.bfloat16).astype(jnp.float32)
                conv[pl.ds(pl.multiple_of((first + t) * tiles, tiles), tiles), :] = value

        @pl.when(least[b] >= K - 1)
        def _():
            totals = [bias[...] for _ in range(BLOCK)]
            for i in range(BLOCK + K - 1):
                row = row_at(first + HALO - (K - 1) + i)
                for t in range(BLOCK):
                    back = t + K - 1 - i
                    if 0 <= back < K:
                        totals[t] = totals[t] + tap(K - 1 - back) * row
            finish(totals)

        @pl.when(least[b] < K - 1)
        def _():
            totals = [bias[...] for _ in range(BLOCK)]
            reach = [jnp.full((tiles, LANES), since[first + t], jnp.int32) for t in range(BLOCK)]
            for i in range(BLOCK + K - 1):
                row = row_at(first + HALO - (K - 1) + i)
                for t in range(BLOCK):
                    back = t + K - 1 - i
                    if 0 <= back < K:
                        kept = jnp.where(reach[t] >= back, row, 0.0)
                        totals[t] = totals[t] + tap(K - 1 - back) * kept
            finish(totals)

        return carry

    lax.fori_loop(0, count // BLOCK, convolve, 0)

    rows = 16

    def normalise(b, carry):
        base = b * (rows * tiles)
        parts = [conv[pl.ds(base + j, rows, stride=tiles), :] for j in range(tiles)]
        total = functools.reduce(jnp.add, parts)
        mean = jnp.sum(total, axis=1, keepdims=True) * (1.0 / width)
        off = [p - mean for p in parts]
        square = functools.reduce(jnp.add, [o * o for o in off])
        var = jnp.sum(square, axis=1, keepdims=True) * (1.0 / width)
        scale = lax.rsqrt(var + 1e-05)
        for j in range(tiles):
            cols = slice(j * LANES, (j + 1) * LANES)
            v = off[j] * scale * gain[:, cols] + nbias[:, cols]
            v = v * jax.nn.sigmoid(v)
            act[pl.ds(pl.multiple_of(b * rows, rows), rows), cols] = v.astype(jnp.bfloat16)
        return carry

    lax.fori_loop(0, count // rows, normalise, 0)


def out_kernel(layout, place, act, *rest):
    npieces = sum(len(block) for block in layout)
    pieces = rest[:npieces]
    out, w, stage, sems, osems = rest[npieces:]
    block_cols = w.shape[2]
    groups = []
    at = 0
    for n, block in enumerate(layout):
        copies = []
        for flip, base, pitch, size in block:
            side = 1 - place[2] if flip else place[2]
            row = pl.multiple_of(side * pitch + base, 16)
            copies.append(pltpu.make_async_copy(pieces[at], w.at[n, pl.ds(row, size)], sems.at[at]))
            at += 1
        groups.append(copy_all(copies))
    outs = []
    near = place[0] * 2 + place[1]
    far = (1 - place[0]) * 2 + place[1]
    swap = 1 - 2 * place[1]
    shards = [near, near + swap, far, far + swap]
    for n in range(len(layout)):
        wait_all(groups[n])
        stage[n] = dot(act[...], w[n]).astype(jnp.bfloat16)
        col = pl.multiple_of(shards[n] * block_cols, block_cols)
        copy = pltpu.make_async_copy(stage.at[n], out.at[:, pl.ds(col, block_cols)], osems.at[n])
        copy.start()
        outs.append(copy)
    wait_all(outs)


def permuted(value, sp, dp, flip_sp, flip_dp):
    pairs = [(s * dp + d, (s ^ flip_sp) * dp + (d ^ flip_dp)) for s in range(sp) for d in range(dp)]
    return lax.ppermute(value, AXES, pairs)


def two_link_body(sp, dp, tokens, segments, w_lin, w_gate, w_out, conv_kernel, conv_bias, norm_gain, norm_bias):
    rows = tokens[0]
    doc_ids = segments[0]
    count, depth = rows.shape
    shard, width = w_lin.shape
    reach = K - 1
    tiles = width // LANES
    s, d = lax.axis_index("sp"), lax.axis_index("dp")
    side = s % 2
    place = jnp.stack([d // 2, d % 2, side]).astype(jnp.int32)

    over_y = lambda v: permuted(v, sp, dp, 0, 2)
    over_x = lambda v: permuted(v, sp, dp, 1, 0)
    over_core = lambda v: permuted(v, sp, dp, 0, 1)

    part = shard * 3 // 16
    pitch = 2 * part
    rest_at = 2 * pitch
    cut = lambda v, at, n: lax.dynamic_slice_in_dim(v, at, n, 0)
    far = {}
    for name, v in (("l", w_lin), ("g", w_gate)):
        a = over_y(cut(v, side * pitch, part))
        b = over_y(cut(v, side * pitch + part, part))
        r = over_y(v[rest_at:])
        far[name] = [a, b, r, over_x(a), over_x(b)]
        far[name] += [over_core(p) for p in far[name]]
    lg_layout = []
    for swap in (0, 1):
        lg_layout += [
            (swap, 0, 0, pitch, part),
            (swap, 0, part, pitch, part),
            (swap, 0, rest_at, 0, shard - rest_at),
            (swap, 1, 0, pitch, part),
            (swap, 1, part, pitch, part),
        ]
    opart = width // 3 // 16 * 16
    orest = 2 * opart
    oa = over_y(cut(w_out, side * opart, opart))
    orr = over_y(w_out[orest:])
    ofar = [oa, orr, over_x(oa)]
    ofar = ofar + [over_core(p) for p in ofar]
    o_block = [(0, 0, opart, opart), (0, orest, 0, width - orest), (1, 0, opart, opart)]
    whole = [(0, 0, 0, width)]

    forward = lambda v: lax.ppermute(v, "sp", [(i, i + 1) for i in range(sp - 1)])
    halo = forward(rows[count - HALO :])
    ids = jnp.concatenate([forward(doc_ids[count - reach :]), doc_ids])
    spot = lax.iota(jnp.int32, count + reach)
    change = jnp.concatenate([jnp.ones((1,), jnp.bool_), ids[1:] != ids[:-1]])
    since = (spot - lax.cummax(jnp.where(change, spot, 0), axis=0))[reach:]
    least = jnp.min(since.reshape(count // BLOCK, BLOCK), axis=1)

    l1, g1, o1 = over_core(w_lin), over_core(w_gate), over_core(w_out)

    ext = count + HALO
    limit = pltpu.CompilerParams(vmem_limit_bytes=48 * 1024 * 1024)
    acc = pl.pallas_call(
        near_kernel,
        out_shape=jax.ShapeDtypeStruct((ext, 2 * width), jnp.float32),
        in_specs=[SMEM] + [ANY] * 6,
        out_specs=VMEM,
        scratch_shapes=[
            pltpu.VMEM((ext, 2 * shard), jnp.bfloat16),
            pltpu.VMEM((2 * shard, 2 * width), jnp.bfloat16),
            pltpu.SemaphoreType.DMA((6,)),
        ],
        compiler_params=limit,
        name="near",
    )(place, rows, halo, w_lin, w_gate, l1, g1)

    pieces = [far[n][i] for i in range(len(lg_layout)) for n in ("l", "g")]
    act = pl.pallas_call(
        functools.partial(far_kernel, lg_layout),
        out_shape=jax.ShapeDtypeStruct((count, width), jnp.bfloat16),
        in_specs=[SMEM] * 3 + [ANY] * 2 + [VMEM] * 5 + [ANY] * len(pieces),
        out_specs=VMEM,
        scratch_shapes=[
            pltpu.VMEM((ext, 2 * shard), jnp.bfloat16),
            pltpu.VMEM((2 * shard, 2 * width), jnp.bfloat16),
            pltpu.VMEM((ext * tiles, LANES), jnp.float32),
            pltpu.VMEM((count * tiles, LANES), jnp.float32),
            pltpu.SemaphoreType.DMA((2 + len(pieces),)),
        ],
        compiler_params=limit,
        name="far",
    )(
        place,
        since,
        least,
        rows,
        halo,
        acc,
        conv_kernel.reshape(K * tiles, LANES),
        conv_bias.reshape(tiles, LANES),
        norm_gain.reshape(1, width),
        norm_bias.reshape(1, width),
        *pieces,
    )

    o_layout = [whole, whole, o_block, o_block]
    o_pieces = [w_out, o1] + ofar
    block_cols = w_out.shape[1]
    out = pl.pallas_call(
        functools.partial(out_kernel, o_layout),
        out_shape=jax.ShapeDtypeStruct((count, depth), jnp.bfloat16),
        in_specs=[SMEM, VMEM] + [ANY] * len(o_pieces),
        out_specs=ANY,
        scratch_shapes=[
            pltpu.VMEM((len(o_layout), width, block_cols), jnp.bfloat16),
            pltpu.VMEM((len(o_layout), count, block_cols), jnp.bfloat16),
            pltpu.SemaphoreType.DMA((len(o_pieces),)),
            pltpu.SemaphoreType.DMA((len(o_layout),)),
        ],
        compiler_params=limit,
        name="mix",
    )(place, act, *o_pieces)
    return out[None]


def solution(mesh):
    sp, dp = mesh.shape["sp"], mesh.shape["dp"]
    body = functools.partial(two_link_body, sp, dp) if dp == 4 and sp % 2 == 0 else plain_body
    placed = (
        P("dp", "sp", None),
        P("dp", "sp"),
        P("dp", None),
        P("dp", None),
        P(None, "dp"),
        P(),
        P(),
        P(),
        P(),
    )
    return jax.shard_map(
        body, mesh=mesh, in_specs=placed, out_specs=P("dp", "sp", None), check_vma=False
    )
```
